32 devices in a mesh: fs: 8 (over z, y), tp: 4 (over x, core).
Axes of the slice: x: 2, y: 2, z: 4, core: 2. Of those that a mesh axis runs over, the one named last changes fastest.
Arguments:
- tokens: bfloat16 [8192, 2048], P('fs'), may hold values from -6 to 6
- w_gate_side: bfloat16 [2048, 1024], P('fs', 'tp'), may hold values from -0.125 to 0.125
- w_value_side: bfloat16 [2048, 1024], P('fs', 'tp'), may hold values from -0.125 to 0.125
- spatial_gain: float32 [1024], P('tp'), may hold values from 0.1 to 1.9
- w_spatial: bfloat16 [16, 128, 128], P('tp'), may hold values from -0.5 to 0.5
- spatial_bias: float32 [16, 128], P('tp'), may hold values from 0.1 to 1.9
- w_mixer_out: bfloat16 [1024, 2048], P('tp', 'fs'), may hold values from -0.1875 to 0.1875
- first_gain: float32 [2048], replicated, may hold values from 0.1 to 1.9
- w_ff_gate: bfloat16 [2048, 5632], P('fs', 'tp'), may hold values from -0.125 to 0.125
- w_ff_up: bfloat16 [2048, 5632], P('fs', 'tp'), may hold values from -0.125 to 0.125
- conv_gate_taps: float32 [3, 5632], P(None, 'tp'), may hold values from -3.5 to 3.5
- conv_up_taps: float32 [3, 5632], P(None, 'tp'), may hold values from -3.5 to 3.5
- w_ff_down: bfloat16 [5632, 2048], P('tp', 'fs'), may hold values from -0.078125 to 0.078125
- second_gain: float32 [2048], replicated, may hold values from 0.1 to 1.9
Outputs:
- layer_out: bfloat16 [8192, 2048], P('fs', 'tp')
The draws below stay inside these ranges and needn't reach their ends.
All inputs are finite; a program needn't handle non-finite values.
Results may differ from the reference program's by a relative error of at most 0.015.
Values may be sent and summed in bfloat16 or wider, within the bound.
A program may use at most 64 MiB of HBM per device.

```python
import jax
import jax.numpy as jnp
from jax import lax

D = 2048
GROUPS = 16
GROUP_DIM = 64
SG_WIDTH = 1024
FF = 5632
SPAN = 128
SEQ = 256
TOKENS = 8192
N_TP = 4


def steps_of(stream_key, shape, split, least, high):
    def one(axis_at, blocks):
        steps = jax.random.uniform(jax.random.fold_in(jax.random.fold_in(stream_key, 6), axis_at), (blocks,), jnp.float32, least / len(split), high / len(split))
        return jnp.repeat(jnp.exp(steps), shape[axis_at] // blocks).reshape((-1,) + (1,) * (len(shape) - axis_at - 1))

    level = one(*split[0])
    for cut in split[1:]:
        level = level * one(*cut)
    return level


def noise(key, shape, scale, limit, shards=(), kind=jnp.bfloat16):
    level = steps_of(key, shape, shards, -0.22, 0.18) if shards else 1.0
    values = jax.random.normal(key, shape, jnp.float32) * scale * level
    return jnp.minimum(jnp.maximum(values, -limit), limit).astype(kind)


def setup_inputs(seed: int = 0) -> dict:
    key_of = jax.random.split(jax.random.key(seed), 15)
    tokens = noise(key_of[0], (TOKENS, D), 1.0, 6.0, ((0, 8),))
    w_gate_side = noise(key_of[1], (D, SG_WIDTH), D ** -0.5, 0.125, ((0, 8), (1, 4)))
    w_value_side = noise(key_of[2], (D, SG_WIDTH), D ** -0.5, 0.125, ((0, 8), (1, 4)))
    spatial_gain = jnp.clip(1.0 + 0.18 * jax.random.normal(key_of[3], (SG_WIDTH,), jnp.float32), 0.1, 1.9)
    w_spatial = noise(key_of[4], (GROUPS, SPAN, SPAN), SPAN ** -0.5, 0.5, ((0, 4),))
    spatial_bias = jnp.clip(1.0 + 0.18 * jax.random.normal(key_of[5], (GROUPS, SPAN), jnp.float32), 0.1, 1.9)
    w_mixer_out = noise(key_of[6], (SG_WIDTH, D), SG_WIDTH ** -0.5, 0.1875, ((0, 4), (1, 8)))
    first_gain = jnp.clip(1.0 + 0.18 * jax.random.normal(key_of[7], (D,), jnp.float32), 0.1, 1.9)
    w_ff_gate = noise(key_of[8], (D, FF), D ** -0.5, 0.125, ((0, 8), (1, 4)))
    w_ff_up = noise(key_of[9], (D, FF), D ** -0.5, 0.125, ((0, 8), (1, 4)))
    conv_gate_taps = noise(key_of[10], (3, FF), 3 ** -0.5, 3.5, ((1, 4),), jnp.float32)
    conv_up_taps = noise(key_of[11], (3, FF), 3 ** -0.5, 3.5, ((1, 4),), jnp.float32)
    w_ff_down = noise(key_of[12], (FF, D), FF ** -0.5, 0.078125, ((0, 4), (1, 8)))
    second_gain = jnp.clip(1.0 + 0.18 * jax.random.normal(key_of[13], (D,), jnp.float32), 0.1, 1.9)
    return {"tokens": tokens, "w_gate_side": w_gate_side, "w_value_side": w_value_side, "spatial_gain": spatial_gain, "w_spatial": w_spatial, "spatial_bias": spatial_bias, "w_mixer_out": w_mixer_out, "first_gain": first_gain, "w_ff_gate": w_ff_gate, "w_ff_up": w_ff_up, "conv_gate_taps": conv_gate_taps, "conv_up_taps": conv_up_taps, "w_ff_down": w_ff_down, "second_gain": second_gain}


residual_scale = 2.0 ** 0.25
norm_eps = 1e-05

def row_norm(values, gain):
    width = values.shape[-1]
    mean = lax.optimization_barrier(jnp.sum(values, axis=-1, keepdims=True)) / width
    square = lax.optimization_barrier(jnp.sum(values * values, axis=-1, keepdims=True)) / width
    spread = square - mean * mean
    return (values - mean) * lax.rsqrt(spread + norm_eps) * gain

def causal_taps(pre, taps):
    count = pre.shape[0] // SEQ
    blocks = pre.reshape(count, SEQ, pre.shape[1])
    padded = jnp.pad(blocks, ((0, 0), (2, 0), (0, 0)))
    result = padded[:, 0:SEQ] * taps[0] + padded[:, 1:SEQ + 1] * taps[1] + padded[:, 2:] * taps[2]
    return result.reshape(pre.shape)

def range_sum(left, right, parts):
    width = left.shape[1] // parts
    total = jnp.zeros((left.shape[0], right.shape[1]), jnp.float32)
    for index in range(parts):
        term = jnp.dot(left[:, index * width:(index + 1) * width], right[index * width:(index + 1) * width], preferred_element_type=jnp.float32)
        total = total + term.astype(jnp.bfloat16).astype(jnp.float32)
    return total

def reference(tokens, w_gate_side, w_value_side, spatial_gain, w_spatial, spatial_bias, w_mixer_out, first_gain, w_ff_gate, w_ff_up, conv_gate_taps, conv_up_taps, w_ff_down, second_gain):
    gate_act = jax.nn.gelu(jnp.dot(tokens, w_gate_side, preferred_element_type=jnp.float32))
    value_act = jax.nn.gelu(jnp.dot(tokens, w_value_side, preferred_element_type=jnp.float32))
    value_norm = row_norm(value_act, spatial_gain).astype(jnp.bfloat16)
    blocks = value_norm.reshape(TOKENS // SPAN, SPAN, GROUPS, GROUP_DIM).astype(jnp.float32)
    lower = jnp.tril(jnp.ones((SPAN, SPAN), jnp.float32))
    causal_w = w_spatial.astype(jnp.float32) * lower
    mixed = jnp.einsum('gts,nsgc->ntgc', causal_w, blocks) + spatial_bias.T[None, :, :, None]
    spatial_out = (gate_act * mixed.reshape(TOKENS, SG_WIDTH)).astype(jnp.bfloat16)
    mixer_sum = range_sum(spatial_out, w_mixer_out, N_TP)
    first_normed = row_norm(residual_scale * tokens.astype(jnp.float32) + mixer_sum, first_gain).astype(jnp.bfloat16)
    ff_gate = causal_taps(jnp.dot(first_normed, w_ff_gate, preferred_element_type=jnp.float32), conv_gate_taps)
    ff_up = causal_taps(jnp.dot(first_normed, w_ff_up, preferred_element_type=jnp.float32), conv_up_taps)
    ff_hidden = (jax.nn.silu(ff_gate) * ff_up).astype(jnp.bfloat16)
    ff_sum = range_sum(ff_hidden, w_ff_down, N_TP)
    layer_out = row_norm(residual_scale * first_normed.astype(jnp.float32) + ff_sum, second_gain)
    return layer_out.astype(jnp.bfloat16)
```

```python
import jax
import jax.numpy as jnp
from jax import lax
from jax.sharding import PartitionSpec as P

GROUP_DIM = 64
SPAN = 128
SEQ = 256
Z = 4
CORES = 2

residual_scale = 2.0**0.25
norm_eps = 1e-05


def fs_pairs(n_fs, dz, dy):
    n_y = n_fs // Z
    pairs = []
    for index in range(n_fs):
        z, y = index // n_y, index % n_y
        pairs.append((index, (z + dz) % Z * n_y + (y + dy) % n_y))
    return pairs


def tp_pairs(n_tp, dx, dc):
    n_x = n_tp // CORES
    pairs = []
    for index in range(n_tp):
        x, c = index // CORES, index % CORES
        pairs.append((index, (x + dx) % n_x * CORES + (c + dc) % CORES))
    return pairs


def move_fs(value, dz, dy):
    return lax.ppermute(value, "fs", fs_pairs(lax.axis_size("fs"), dz, dy))


def move_tp(value, dx, dc):
    return lax.ppermute(value, "tp", tp_pairs(lax.axis_size("tp"), dx, dc))


def y_blocks(own):
    n_y = lax.axis_size("fs") // Z
    y = lax.axis_index("fs") % n_y
    pieces = [own]
    for step in range(1, n_y):
        pieces.append(move_fs(pieces[-1], 0, 1))
    return [lax.select_n((y - at) % n_y, *pieces) if n_y > 2 else lax.select_n((y - at) % n_y == 1, *pieces) for at in range(n_y)]


def z_ring(own):
    right = move_fs(own, 1, 0)
    left = move_fs(own, -1, 0)
    far = move_fs(right, 1, 0)
    return [own, left, far, right]


def row_norm(values, gain):
    width = values.shape[1]
    mean = jnp.sum(values, axis=1, keepdims=True) / width
    spread = jnp.sum(values * values, axis=1, keepdims=True) / width - mean * mean
    return (values - mean) * lax.rsqrt(spread + norm_eps) * gain


def scatter_rows(part):
    n_tp = lax.axis_size("tp")
    n_x = n_tp // CORES
    tp = lax.axis_index("tp")
    x, c = tp // CORES, tp % CORES
    rows, cols = part.shape
    blocks = part.astype(jnp.bfloat16).reshape(n_x, CORES, rows // n_tp, cols)
    mine = lax.dynamic_index_in_dim(blocks, c, 1, keepdims=False)
    other = lax.dynamic_index_in_dim(blocks, 1 - c, 1, keepdims=False)
    pair = mine.astype(jnp.float32) + move_tp(other, 0, 1).astype(jnp.float32)
    total = lax.dynamic_index_in_dim(pair, x, 0, keepdims=False)
    for dx in range(1, n_x):
        away = lax.dynamic_index_in_dim(pair, (x + dx) % n_x, 0, keepdims=False)
        total = total + move_tp(away.astype(jnp.bfloat16), dx, 0).astype(jnp.float32)
    return total


def gather_rows(own):
    n_tp = lax.axis_size("tp")
    n_x = n_tp // CORES
    tp = lax.axis_index("tp")
    x, c = tp // CORES, tp % CORES
    column = [own]
    for dx in range(1, n_x):
        column.append(move_tp(own, dx, 0))
    column_abs = [
        lax.select_n((x - at) % n_x == 1, *column) if n_x == 2 else lax.select_n((x - at) % n_x, *column)
        for at in range(n_x)
    ]
    near = [move_tp(value, 0, 1) for value in column]
    near_abs = [
        lax.select_n((x - at) % n_x == 1, *near) if n_x == 2 else lax.select_n((x - at) % n_x, *near)
        for at in range(n_x)
    ]
    pieces = []
    for at in range(n_x):
        pieces.append(jnp.where(c == 0, column_abs[at], near_abs[at]))
        pieces.append(jnp.where(c == 0, near_abs[at], column_abs[at]))
    return jnp.concatenate(pieces, axis=0)


def rows_to_columns(own):
    n_tp = lax.axis_size("tp")
    n_x = n_tp // CORES
    tp = lax.axis_index("tp")
    x, c = tp // CORES, tp % CORES
    rows, cols = own.shape
    width = cols // n_tp
    result = jnp.zeros((n_tp * rows, width), own.dtype)
    for dx in range(n_x):
        for dc in range(CORES):
            to = (x + dx) % n_x * CORES + (c + dc) % CORES
            came = (x - dx) % n_x * CORES + (c - dc) % CORES
            block = lax.dynamic_slice_in_dim(own, to * width, width, 1)
            if dx or dc:
                block = move_tp(block, dx, dc)
            result = lax.dynamic_update_slice_in_dim(result, block, came * rows, 0)
    return result


def causal_taps(pre, taps):
    count = pre.shape[0] // SEQ
    blocks = pre.reshape(count, SEQ, pre.shape[1])
    padded = jnp.pad(blocks, ((0, 0), (2, 0), (0, 0)))
    result = padded[:, 0:SEQ] * taps[0] + padded[:, 1 : SEQ + 1] * taps[1] + padded[:, 2:] * taps[2]
    return result.reshape(pre.shape)


def mm(left, right):
    return jnp.dot(left, right, preferred_element_type=jnp.float32)


def split_norm(values, gain, width):
    sums = jnp.stack([jnp.sum(values, axis=1), jnp.sum(values * values, axis=1)])
    n_x = lax.axis_size("tp") // CORES
    total = sums
    for dx in range(n_x):
        for dc in range(CORES):
            if dx or dc:
                total = total + move_tp(sums, dx, dc)
    mean = total[0][:, None] / width
    spread = total[1][:, None] / width - mean * mean
    return (values - mean) * lax.rsqrt(spread + norm_eps) * gain


def per_device(
    tokens,
    w_gate_side,
    w_value_side,
    spatial_gain,
    w_spatial,
    spatial_bias,
    w_mixer_out,
    first_gain,
    w_ff_gate,
    w_ff_up,
    conv_gate_taps,
    conv_up_taps,
    w_ff_down,
    second_gain,
):
    rows, d = tokens.shape
    n_fs, n_tp = lax.axis_size("fs"), lax.axis_size("tp")
    n_y = n_fs // Z
    z = lax.axis_index("fs") // n_y
    tp = lax.axis_index("tp")
    shift = z * (d // Z)
    own_rows = rows // n_tp
    side = w_gate_side.shape[1]
    depth = w_gate_side.shape[0]

    near = y_blocks(jnp.concatenate([w_gate_side, w_value_side], axis=1))
    near_mix = y_blocks(w_mixer_out)
    sides = z_ring(jnp.concatenate(near, axis=0))
    mixes = z_ring(jnp.concatenate(near_mix, axis=1))
    gate_z = z_ring(w_ff_gate)
    gate_w = jnp.concatenate([b for s in gate_z for b in y_blocks(s)], axis=0)
    up_z = z_ring(w_ff_up)
    up_w = jnp.concatenate([b for s in up_z for b in y_blocks(s)], axis=0)
    down_z = z_ring(w_ff_down)
    down_w = [jnp.concatenate(y_blocks(s), axis=1) for s in down_z]

    tokens_rel = jnp.roll(tokens, -shift, axis=1)
    pre = mm(tokens_rel, jnp.concatenate(sides, axis=0))
    gate_act = jax.nn.gelu(pre[:, :side])
    value_norm = split_norm(
        jax.nn.gelu(pre[:, side:]), spatial_gain, side * n_tp
    ).astype(jnp.bfloat16)
    groups_dev = w_spatial.shape[0]
    blocks = value_norm.reshape(rows // SPAN, SPAN, groups_dev, GROUP_DIM)
    lower = jnp.tril(jnp.ones((SPAN, SPAN), jnp.bool_))
    causal_w = jnp.where(lower[None], w_spatial, jnp.zeros_like(w_spatial))
    mixed = jnp.einsum("gts,nsgc->ntgc", causal_w, blocks, preferred_element_type=jnp.float32)
    mixed = mixed + spatial_bias.T[None, :, :, None]
    spatial_out = (gate_act * mixed.reshape(rows, side)).astype(jnp.bfloat16)
    mixer_sum = scatter_rows(mm(spatial_out, jnp.concatenate(mixes, axis=1)))
    own_tokens = lax.dynamic_slice_in_dim(tokens_rel, tp * own_rows, own_rows, 0)
    first_own = row_norm(
        residual_scale * own_tokens.astype(jnp.float32) + mixer_sum, jnp.roll(first_gain, -shift)
    ).astype(jnp.bfloat16)
    first_whole = gather_rows(first_own)

    ff_gate = causal_taps(mm(first_whole, gate_w), conv_gate_taps)
    ff_up = causal_taps(mm(first_whole, up_w), conv_up_taps)
    ff_hidden = (jax.nn.silu(ff_gate) * ff_up).astype(jnp.bfloat16)
    ff_sum = jnp.concatenate([scatter_rows(mm(ff_hidden, piece)) for piece in down_w], axis=1)
    out_rel = row_norm(
        residual_scale * first_own.astype(jnp.float32) + ff_sum, jnp.roll(second_gain, -shift)
    ).astype(jnp.bfloat16)
    return rows_to_columns(jnp.roll(out_rel, shift, axis=1))


def solution(mesh):
    return jax.shard_map(
        per_device,
        mesh=mesh,
        in_specs=(
            P("fs", None),
            P("fs", "tp"),
            P("fs", "tp"),
            P("tp"),
            P("tp", None, None),
            P("tp", None),
            P("tp", "fs"),
            P(),
            P("fs", "tp"),
            P("fs", "tp"),
            P(None, "tp"),
            P(None, "tp"),
            P("tp", "fs"),
            P(),
        ),
        out_specs=P("fs", "tp"),
        check_vma=False,
    )
```

```python
import jax
import jax.numpy as jnp
from jax import lax
from jax.sharding import PartitionSpec as P

GROUP_DIM = 64
SPAN = 128
SEQ = 256
Z = 4
CORES = 2

residual_scale = 2.0**0.25
norm_eps = 1e-05


def fs_pairs(n_fs, dz, dy):
    n_y = n_fs // Z
    pairs = []
    for index in range(n_fs):
        z, y = index // n_y, index % n_y
        pairs.append((index, (z + dz) % Z * n_y + (y + dy) % n_y))
    return pairs


def tp_pairs(n_tp, dx, dc):
    n_x = n_tp // CORES
    pairs = []
    for index in range(n_tp):
        x, c = index // CORES, index % CORES
        pairs.append((index, (x + dx) % n_x * CORES + (c + dc) % CORES))
    return pairs


def move_fs(value, dz, dy):
    return lax.ppermute(value, "fs", fs_pairs(lax.axis_size("fs"), dz, dy))


def move_tp(value, dx, dc):
    return lax.ppermute(value, "tp", tp_pairs(lax.axis_size("tp"), dx, dc))


def y_blocks(own):
    n_y = lax.axis_size("fs") // Z
    y = lax.axis_index("fs") % n_y
    pieces = [own]
    for step in range(1, n_y):
        pieces.append(move_fs(pieces[-1], 0, 1))
    return [lax.select_n((y - at) % n_y, *pieces) if n_y > 2 else lax.select_n((y - at) % n_y == 1, *pieces) for at in range(n_y)]


def after(value, *earlier):
    return lax.optimization_barrier((value, *earlier))[0]


def z_near(own):
    return move_fs(own, -1, 0), move_fs(own, 1, 0)


def z_ring(own):
    left, right = z_near(own)
    return [own, left, move_fs(right, 1, 0), right]


def row_norm(values, gain):
    width = values.shape[1]
    mean = jnp.sum(values, axis=1, keepdims=True) / width
    spread = jnp.sum(values * values, axis=1, keepdims=True) / width - mean * mean
    return (values - mean) * lax.rsqrt(spread + norm_eps) * gain


def scatter_rows(part):
    n_tp = lax.axis_size("tp")
    n_x = n_tp // CORES
    tp = lax.axis_index("tp")
    x, c = tp // CORES, tp % CORES
    rows, cols = part.shape
    blocks = part.astype(jnp.bfloat16).reshape(n_x, CORES, rows // n_tp, cols)
    mine = lax.dynamic_index_in_dim(blocks, c, 1, keepdims=False)
    other = lax.dynamic_index_in_dim(blocks, 1 - c, 1, keepdims=False)
    pair = mine.astype(jnp.float32) + move_tp(other, 0, 1).astype(jnp.float32)
    total = lax.dynamic_index_in_dim(pair, x, 0, keepdims=False)
    for dx in range(1, n_x):
        away = lax.dynamic_index_in_dim(pair, (x + dx) % n_x, 0, keepdims=False).astype(jnp.bfloat16)
        total = total + move_tp(away, dx, 0).astype(jnp.float32)
    return total, away


def gather_rows(own):
    n_tp = lax.axis_size("tp")
    n_x = n_tp // CORES
    tp = lax.axis_index("tp")
    x, c = tp // CORES, tp % CORES
    column = [own]
    for dx in range(1, n_x):
        column.append(move_tp(own, dx, 0))
    column_abs = [
        lax.select_n((x - at) % n_x == 1, *column) if n_x == 2 else lax.select_n((x - at) % n_x, *column)
        for at in range(n_x)
    ]
    near = [move_tp(value, 0, 1) for value in column]
    near_abs = [
        lax.select_n((x - at) % n_x == 1, *near) if n_x == 2 else lax.select_n((x - at) % n_x, *near)
        for at in range(n_x)
    ]
    pieces = []
    for at in range(n_x):
        pieces.append(jnp.where(c == 0, column_abs[at], near_abs[at]))
        pieces.append(jnp.where(c == 0, near_abs[at], column_abs[at]))
    return jnp.concatenate(pieces, axis=0), column[-1]


def rows_to_columns(own):
    n_tp = lax.axis_size("tp")
    n_x = n_tp // CORES
    tp = lax.axis_index("tp")
    x, c = tp // CORES, tp % CORES
    rows, cols = own.shape
    width = cols // n_tp
    result = jnp.zeros((n_tp * rows, width), own.dtype)
    for dx in range(n_x):
        for dc in range(CORES):
            to = (x + dx) % n_x * CORES + (c + dc) % CORES
            came = (x - dx) % n_x * CORES + (c - dc) % CORES
            block = lax.dynamic_slice_in_dim(own, to * width, width, 1)
            if dx or dc:
                block = move_tp(block, dx, dc)
            result = lax.dynamic_update_slice_in_dim(result, block, came * rows, 0)
    return result


def causal_taps(pre, taps):
    count = pre.shape[0] // SEQ
    blocks = pre.reshape(count, SEQ, pre.shape[1])
    padded = jnp.pad(blocks, ((0, 0), (2, 0), (0, 0)))
    result = padded[:, 0:SEQ] * taps[0] + padded[:, 1 : SEQ + 1] * taps[1] + padded[:, 2:] * taps[2]
    return result.reshape(pre.shape)


def mm(left, right):
    return jnp.dot(left, right, preferred_element_type=jnp.float32)


def split_norm(values, gain, width):
    sums = jnp.stack([jnp.sum(values, axis=1), jnp.sum(values * values, axis=1)])
    n_x = lax.axis_size("tp") // CORES
    total = sums
    for dx in range(n_x):
        for dc in range(CORES):
            if dx or dc:
                total = total + move_tp(sums, dx, dc)
    mean = total[0][:, None] / width
    spread = total[1][:, None] / width - mean * mean
    return (values - mean) * lax.rsqrt(spread + norm_eps) * gain


def per_device(
    tokens,
    w_gate_side,
    w_value_side,
    spatial_gain,
    w_spatial,
    spatial_bias,
    w_mixer_out,
    first_gain,
    w_ff_gate,
    w_ff_up,
    conv_gate_taps,
    conv_up_taps,
    w_ff_down,
    second_gain,
):
    rows, d = tokens.shape
    n_fs, n_tp = lax.axis_size("fs"), lax.axis_size("tp")
    n_y = n_fs // Z
    z = lax.axis_index("fs") // n_y
    tp = lax.axis_index("tp")
    shift = z * (d // Z)
    own_rows = rows // n_tp
    side = w_gate_side.shape[1]
    depth = w_gate_side.shape[0]

    near = y_blocks(jnp.concatenate([w_gate_side, w_value_side], axis=1))
    near_mix = y_blocks(w_mixer_out)
    sides = z_ring(jnp.concatenate(near, axis=0))
    mixes = z_ring(after(jnp.concatenate(near_mix, axis=1), sides[1], sides[3]))
    started = (near[-1], near_mix[-1])
    own_gate, own_up, own_down = (after(w, *started) for w in (w_ff_gate, w_ff_up, w_ff_down))
    own_blocks = [y_blocks(w) for w in (own_gate, own_up, own_down)]
    gate_near = z_near(after(own_gate, sides[1], sides[3]))
    gate_far = move_fs(gate_near[1], 1, 0)
    up_near = z_near(after(own_up, *gate_near))
    gate_sides = [y_blocks(w) for w in gate_near]

    tokens_rel = jnp.roll(tokens, -shift, axis=1)
    pre = mm(tokens_rel, jnp.concatenate(sides, axis=0))
    gate_act = jax.nn.gelu(pre[:, :side])
    value_norm = split_norm(
        jax.nn.gelu(pre[:, side:]), spatial_gain, side * n_tp
    ).astype(jnp.bfloat16)
    groups_dev = w_spatial.shape[0]
    blocks = value_norm.reshape(rows // SPAN, SPAN, groups_dev, GROUP_DIM)
    lower = jnp.tril(jnp.ones((SPAN, SPAN), jnp.bool_))
    causal_w = jnp.where(lower[None], w_spatial, jnp.zeros_like(w_spatial))
    mixed = jnp.einsum("gts,nsgc->ntgc", causal_w, blocks, preferred_element_type=jnp.float32)
    mixed = mixed + spatial_bias.T[None, :, :, None]
    spatial_out = (gate_act * mixed.reshape(rows, side)).astype(jnp.bfloat16)
    mixer_sum, away = scatter_rows(mm(spatial_out, jnp.concatenate(mixes, axis=1)))
    up_near = after(up_near[0], away), after(up_near[1], away)
    up_far = move_fs(up_near[1], 1, 0)
    down_near = z_near(after(own_down, *up_near))
    own_tokens = lax.dynamic_slice_in_dim(tokens_rel, tp * own_rows, own_rows, 0)
    first_own = row_norm(
        residual_scale * own_tokens.astype(jnp.float32) + mixer_sum, jnp.roll(first_gain, -shift)
    ).astype(jnp.bfloat16)
    first_whole, came = gather_rows(first_own)
    gate_opposite = y_blocks(after(gate_far, first_own))
    up_sides = [y_blocks(after(w, came)) for w in up_near]
    up_opposite = y_blocks(after(up_far, came))
    down_near = after(down_near[0], came), after(down_near[1], came)
    down_far = move_fs(down_near[1], 1, 0)
    down_sides = [y_blocks(w) for w in down_near]

    gate_blocks = own_blocks[0] + gate_sides[0] + gate_opposite + gate_sides[1]
    up_blocks = own_blocks[1] + up_sides[0] + up_opposite + up_sides[1]
    gate_w = jnp.concatenate([after(b, came) for b in gate_blocks], axis=0)
    up_w = jnp.concatenate([after(b, first_whole) for b in up_blocks], axis=0)
    ff_gate = causal_taps(mm(first_whole, gate_w), conv_gate_taps)
    down_opposite = y_blocks(after(down_far, first_whole))
    ff_up = causal_taps(mm(first_whole, up_w), conv_up_taps)
    ff_hidden = (jax.nn.silu(ff_gate) * ff_up).astype(jnp.bfloat16)
    sums = {}
    earlier = [ff_hidden, ff_hidden]
    sent = ff_hidden
    for at, piece in ((0, own_blocks[2]), (1, down_sides[0]), (3, down_sides[1]), (2, down_opposite)):
        piece = [after(block, sent, earlier[-2]) for block in piece]
        sums[at], sent = scatter_rows(mm(ff_hidden, jnp.concatenate(piece, axis=1)))
        earlier.append(sums[at])
    ff_sum = jnp.concatenate([sums[at] for at in range(Z)], axis=1)
    out_rel = row_norm(
        residual_scale * first_own.astype(jnp.float32) + ff_sum, jnp.roll(second_gain, -shift)
    ).astype(jnp.bfloat16)
    return rows_to_columns(jnp.roll(out_rel, shift, axis=1))


def solution(mesh):
    return jax.shard_map(
        per_device,
        mesh=mesh,
        in_specs=(
            P("fs", None),
            P("fs", "tp"),
            P("fs", "tp"),
            P("tp"),
            P("tp", None, None),
            P("tp", None),
            P("tp", "fs"),
            P(),
            P("fs", "tp"),
            P("fs", "tp"),
            P(None, "tp"),
            P(None, "tp"),
            P("tp", "fs"),
            P(),
        ),
        out_specs=P("fs", "tp"),
        check_vma=False,
    )
```
